32 devices in a mesh: grp: 2 (over y), sp: 4 (over z), tp: 4 (over x, core).
Axes of the slice: x: 2, y: 2, z: 4, core: 2. Of those that a mesh axis runs over, the one named last changes fastest.
Arguments:
- layer_feed: bfloat16 [4, 2048, 4096], P('grp', 'sp'), parts along dimension 0, may hold values from -13 to 13
- address_mapping: bfloat16 [4096, 2048], P(None, 'tp'), may hold values from -0.09375 to 0.09375
- content_mapping: bfloat16 [4096, 2048], P(None, 'tp'), may hold values from -0.09375 to 0.09375
- beta_mapping_matrix: bfloat16 [4096, 32], replicated, may hold values from -0.032958984 to 0.029541016
- forgetting_mapping: bfloat16 [4096, 32], replicated, may hold values from -0.09375 to 0.09375
- logged_fading_speed: float32 [32], P('tp'), may hold values from -12 to -2.8
- extra_forgetting: bfloat16 [4, 2048, 32], P('grp', 'sp', 'tp'), parts along dimension 0, may hold values from -1.4 to 0
- opening_probe: bfloat16 [4, 2048], P('grp', 'tp'), parts along dimension 0, may hold values from -6 to 6
Outputs:
- context_memory_tensor: bfloat16 [4, 32, 64, 64], P('grp', 'tp', 'sp'), parts along dimension 0
- opening_normed_output: bfloat16 [4, 2048], P('grp', 'tp'), parts along dimension 0
The draws below stay inside these ranges and needn't reach their ends.
There are 2 independent parts, one for each index of `grp`. The reference program is written for one: setup_inputs(seed, part) draws one part's arguments, and reference() takes and returns one part's arrays. A program takes and returns all parts, laid end to end along the dimension named above; an argument that names none is the same for every part. Nothing has to cross between parts.
All inputs are finite; a program needn't handle non-finite values.
Results may differ from the reference program's by a relative error of at most 0.014.
Values sent between devices are 32-bit elements; how exact they have to be, the bound alone decides.
A program may use at most 64 MiB of HBM per device.

```python
import math
import jax
import jax.numpy as jnp
from jax import lax

D = 4096
H = 32
HEAD = 64
SEQS = 2
TOK_DEV = 1024
LEN = 2048


def draw_layer_feed(key, part):
    span = TOK_DEV // SEQS
    count = LEN // span
    normal_key = jax.random.fold_in(key, 11)
    scale_key = jax.random.fold_in(key, 12)
    shift_key = jax.random.fold_in(key, 13)
    base = jnp.clip(jax.random.normal(normal_key, (SEQS, count, span, D), jnp.float32), -4.0, 4.0)
    levels = jnp.exp(jax.random.uniform(scale_key, (SEQS, count, 1, 1), jnp.float32, math.log(0.3), math.log(3.0)))
    shifts = jax.random.uniform(shift_key, (SEQS, 1, 1, 1), jnp.float32, 0.45, 0.55)
    scaled = base * levels + shifts
    return scaled.reshape(SEQS, LEN, D).astype(jnp.bfloat16)


def draw_beta_mapping_matrix(key, part):
    noise_key = jax.random.fold_in(key, 41)
    noise = jnp.clip(jax.random.normal(noise_key, (D, H), jnp.float32), -4.0, 4.0) * 0.5
    return (noise * D ** (-0.5) - 7.0 / D).astype(jnp.bfloat16)


def draw_logged_fading_speed(key, part):
    pick_key = jax.random.fold_in(key, 21)
    slow_key = jax.random.fold_in(key, 22)
    fast_key = jax.random.fold_in(key, 23)
    fast = jax.random.bernoulli(pick_key, 0.5, (H,))
    slow_rate = jax.random.uniform(slow_key, (H,), jnp.float32, 0.1, 0.5) / LEN
    fast_rate = jnp.exp(jax.random.uniform(fast_key, (H,), jnp.float32, math.log(0.03), math.log(0.06)))
    return jnp.log(jnp.where(fast, fast_rate, slow_rate)).astype(jnp.float32)


def draw_extra_forgetting(key, part):
    place_key = jax.random.fold_in(key, 31)
    depth_key = jax.random.fold_in(key, 32)
    spots = jax.random.randint(place_key, (SEQS, 2, 1, H), 0, LEN)
    depths = jnp.log(jax.random.uniform(depth_key, (SEQS, 2, 1, H), jnp.float32, 0.5, 0.8))
    positions = jnp.arange(LEN)[None, None, :, None]
    total = jnp.sum(jnp.where(positions == spots, depths, 0.0), axis=1)
    return total.astype(jnp.bfloat16)


def block_scale(stream_key, shape, cuts, low, top_value):
    loudness = 1.0
    for position, blocks in cuts:
        heights = jax.random.uniform(jax.random.fold_in(jax.random.fold_in(stream_key, 6), position), (blocks,), jnp.float32, low / len(cuts), top_value / len(cuts))
        loudness = loudness * jnp.repeat(jnp.exp(heights), shape[position] // blocks).reshape((-1,) + (1,) * (len(shape) - 1 - position))
    return loudness


def centred(rng, shape, spread, reach, shards=(), held_as=jnp.bfloat16):
    array = spread * jax.random.normal(rng, shape, jnp.float32)
    if shards:
        array = array * block_scale(rng, shape, shards, -0.22, 0.18)
    return jnp.clip(array, -reach, reach).astype(held_as)


def setup_inputs(seed: int = 0, part: int = 0) -> dict:
    streams_of = jax.random.split(jax.random.key(seed), 9)
    part_keys = jax.random.split(jax.random.fold_in(streams_of[8], part), 9)
    layer_feed = draw_layer_feed(jax.random.fold_in(jax.random.fold_in(streams_of[8], part), 71), part)
    address_mapping = centred(streams_of[1], (D, H * HEAD), D ** -0.5, 0.09375, ((1, 4),))
    content_mapping = centred(streams_of[2], (D, H * HEAD), D ** -0.5, 0.09375, ((1, 4),))
    beta_mapping_matrix = draw_beta_mapping_matrix(jax.random.fold_in(streams_of[8], 71), part)
    forgetting_mapping = centred(streams_of[4], (D, H), D ** -0.5, 0.09375)
    logged_fading_speed = draw_logged_fading_speed(jax.random.fold_in(streams_of[8], 71), part)
    extra_forgetting = draw_extra_forgetting(jax.random.fold_in(jax.random.fold_in(streams_of[8], part), 71), part)
    opening_probe = centred(part_keys[7], (SEQS, H * HEAD), 1.0, 6.0, ((1, 4),))
    return dict(layer_feed=layer_feed, address_mapping=address_mapping, content_mapping=content_mapping, beta_mapping_matrix=beta_mapping_matrix, forgetting_mapping=forgetting_mapping, logged_fading_speed=logged_fading_speed, extra_forgetting=extra_forgetting, opening_probe=opening_probe)


def reference(layer_feed, address_mapping, content_mapping, beta_mapping_matrix, forgetting_mapping, logged_fading_speed, extra_forgetting, opening_probe):

    def lone_example(input_tokens):
        sequence_tokens, sequence_batch, sequence_query = input_tokens
        address_embeddings = jnp.dot(sequence_tokens, address_mapping, preferred_element_type=jnp.float32).astype(jnp.bfloat16)
        content_embeddings = jnp.dot(sequence_tokens, content_mapping, preferred_element_type=jnp.float32).astype(jnp.bfloat16)
        beta_raw_scores = jnp.dot(sequence_tokens, beta_mapping_matrix, preferred_element_type=jnp.float32).astype(jnp.bfloat16)
        forgetting_raw_scores = jnp.dot(sequence_tokens, forgetting_mapping, preferred_element_type=jnp.float32).astype(jnp.bfloat16)
        keys = jax.nn.silu(address_embeddings.astype(jnp.float32)).reshape(-1, H, HEAD)
        keys = keys * lax.rsqrt(lax.optimization_barrier(jnp.sum(keys * keys, axis=-1, keepdims=True)) + 1e-06)
        values = jax.nn.silu(content_embeddings.astype(jnp.float32)).reshape(-1, H, HEAD)
        betas = jax.nn.sigmoid(beta_raw_scores.astype(jnp.float32))
        decay_factors = -jnp.exp(logged_fading_speed) * jax.nn.softplus(forgetting_raw_scores.astype(jnp.float32)) + sequence_batch.astype(jnp.float32)

        def advance(state, items):
            key_vector_row, value_row, beta_row, gamma_row = items
            retained = jnp.exp(gamma_row)[:, None, None] * state
            estimate = jnp.einsum('yz,yzt->yt', key_vector_row, retained, precision=lax.Precision.HIGHEST)
            state = retained + (beta_row[:, None] * key_vector_row)[:, :, None] * (value_row - estimate)[:, None, :]
            return (state, None)
        start = jnp.zeros((H, HEAD, HEAD), jnp.float32)
        final, _ = lax.scan(advance, start, (keys, values, betas, decay_factors))
        state_store = final.astype(jnp.bfloat16)
        query_per_head = sequence_query.astype(jnp.float32).reshape(H, HEAD)
        state_readout = jnp.einsum('yz,yzt->yt', query_per_head, final, precision=lax.Precision.HIGHEST)
        state_readout = state_readout * lax.rsqrt(lax.optimization_barrier(jnp.mean(state_readout * state_readout, axis=-1, keepdims=True)) + 1e-06)
        return (state_store, state_readout.reshape(H * HEAD).astype(jnp.bfloat16))
    context_memory_tensor, opening_normed_output = lax.map(lone_example, (layer_feed, extra_forgetting, opening_probe))
    return (context_memory_tensor, opening_normed_output)
```

```python
import functools
import math

import jax
import jax.numpy as jnp
from jax import lax
from jax.experimental import pallas as pl
from jax.experimental.pallas import tpu as pltpu
from jax.sharding import PartitionSpec as P

HEAD = 64
F32 = jnp.float32
BF16 = jnp.bfloat16

finest = lax.Precision.HIGHEST


def mm(left, right):
    return jnp.dot(left, right, preferred_element_type=F32)


def iota(shape, dim):
    return lax.broadcasted_iota(jnp.int32, shape, dim)


def onehot(flag):
    return jnp.where(flag, 1.0, 0.0).astype(BF16)


def lane_masks(pack, width):
    lane_head = iota((1, width), 1) // HEAD
    return [onehot(lane_head == h) for h in range(pack)]


def blockdiag(member, masks):
    return jnp.concatenate([member * mask for mask in masks], axis=0)


def kernel(steps_per_seq, pack, x_ref, wk_ref, wv_ref, wb_ref, wf_ref, speed_ref, extra_ref,
           out_ref, gate_weight, state):
    step = pl.program_id(0)
    rows = x_ref.shape[0]
    columns = wk_ref.shape[1]
    heads = columns // HEAD
    width = pack * HEAD
    quads = columns // width
    chunks = rows // HEAD
    all_heads = wb_ref.shape[1]
    first_head = lax.axis_index("tp") * heads
    masks = lane_masks(pack, width)

    row_c = iota((HEAD, width), 0)
    lane_c = iota((HEAD, width), 1) % HEAD
    below = row_c > lane_c
    diagonal = row_c == lane_c
    apart = row_c ^ lane_c

    @pl.when(step == 0)
    def _():
        source = iota((all_heads, 128), 0)
        lane = iota((all_heads, 128), 1)
        to_beta = onehot((source == first_head + lane) & (lane < heads))
        to_decay = onehot((source == first_head + lane - heads) & (lane >= heads) & (lane < 2 * heads))
        gate_weight[...] = (mm(wb_ref[...], to_beta) + mm(wf_ref[...], to_decay)).astype(BF16)

    @pl.when(lax.rem(step, steps_per_seq) == 0)
    def _():
        eye = jnp.where(diagonal, 1.0, 0.0)
        for quad in range(quads):
            state[quad, :HEAD, :] = jnp.zeros((HEAD, width), F32)
            state[quad, HEAD:, :] = eye

    x = x_ref[...]
    gates = mm(x, gate_weight[...]).astype(BF16)
    key_proj = mm(x, wk_ref[...]).astype(BF16).astype(F32)
    value_proj = mm(x, wv_ref[...]).astype(BF16).astype(F32)

    source = iota((128, columns), 0)
    target = iota((128, columns), 1) // HEAD
    beta_pre = mm(gates, onehot(source == target))
    decay_pre = mm(gates, onehot(source == target + heads))
    source = iota((heads, columns), 0)
    target = iota((heads, columns), 1) // HEAD
    extra = mm(extra_ref[...], onehot(source == target))

    beta = jax.nn.sigmoid(beta_pre)
    softplus = jnp.maximum(decay_pre, 0.0) + jnp.log1p(jnp.exp(-jnp.abs(decay_pre)))
    gamma = speed_ref[...] * softplus + extra
    high = gamma.astype(BF16)
    rest = gamma - high.astype(F32)
    middle = rest.astype(BF16)
    low = (rest - middle.astype(F32)).astype(BF16)
    r_idx = iota((rows, rows), 0)
    c_idx = iota((rows, rows), 1)
    running = onehot((r_idx >= c_idx) & (r_idx // HEAD == c_idx // HEAD))
    cumul = mm(running, high) + mm(running, middle) + mm(running, low)

    key = key_proj * jax.nn.sigmoid(key_proj)
    value = value_proj * jax.nn.sigmoid(value_proj)
    group = onehot(iota((width, width), 0) // HEAD == iota((width, width), 1) // HEAD)
    squares = (key * key).astype(BF16)
    total = jnp.concatenate(
        [mm(squares[:, q * width:(q + 1) * width], group) for q in range(quads)], axis=1)
    key = key * lax.rsqrt(total + 1e-06)

    units = []
    for chunk in range(chunks):
        for quad in range(quads):
            units.append((slice(chunk * HEAD, (chunk + 1) * HEAD), slice(quad * width, (quad + 1) * width)))

    lowers = []
    for rs, cs in units:
        k16 = key[rs, cs].astype(BF16)
        gram = lax.dot_general(k16, blockdiag(k16, masks), (((1,), (1,)), ((), ())),
                               preferred_element_type=F32)
        cum = cumul[rs, cs]
        across = jnp.sum(jnp.where(diagonal, cum, 0.0), axis=0, keepdims=True)
        weights = jnp.exp(jnp.where(below, cum - across, 0.0))
        lowers.append(jnp.where(below, beta[rs, cs] * gram * weights, 0.0))

    inverses = [jnp.where(diagonal, 1.0, jnp.where(apart == 1, -lower, 0.0)) for lower in lowers]
    size = 2
    while size < HEAD:
        inv16 = [inverse.astype(BF16) for inverse in inverses]
        parts = []
        for lower, inverse in zip(lowers, inv16):
            corner = jnp.where((apart >= size) & (apart < 2 * size), lower, 0.0).astype(BF16)
            parts.append(mm(inverse, blockdiag(corner, masks)).astype(BF16))
        inverses = [inverse - mm(part, blockdiag(i16, masks))
                    for inverse, part, i16 in zip(inverses, parts, inv16)]
        size *= 2

    maps = []
    for (rs, cs), inverse in zip(units, inverses):
        i16 = inverse.astype(BF16)
        b, k, cum = beta[rs, cs], key[rs, cs], cumul[rs, cs]
        update = mm(i16, blockdiag((b * value[rs, cs]).astype(BF16), masks))
        mixing = mm(i16, blockdiag((b * jnp.exp(cum) * k).astype(BF16), masks))
        last = cum[HEAD - 1:HEAD, :]
        carried = (k * jnp.exp(last - cum)).astype(BF16)
        contract = (((0,), (0,)), ((), ()))
        offset = lax.dot_general(update.astype(BF16), carried, contract, preferred_element_type=F32)
        erase = lax.dot_general(mixing.astype(BF16), carried, contract, preferred_element_type=F32)
        offset = sum(offset[h * HEAD:(h + 1) * HEAD] * masks[h].astype(F32) for h in range(pack))
        erase = jnp.concatenate(
            [erase[h * HEAD:(h + 1) * HEAD].astype(BF16) * masks[h] for h in range(pack)], axis=0)
        maps.append((jnp.exp(last), erase, offset))

    for quad in range(quads):
        held = state[quad]
        for chunk in range(chunks):
            closing, erase, offset = maps[chunk * quads + quad]
            held = closing * held - mm(held.astype(BF16), erase)
            held = jnp.concatenate([held[:HEAD] + offset, held[HEAD:]], axis=0)
        state[quad] = held

    @pl.when(lax.rem(step, steps_per_seq) == steps_per_seq - 1)
    def _():
        out_ref[0] = state[...]


def device_maps(layer_feed, address_mapping, content_mapping, beta_mapping_matrix,
                forgetting_mapping, logged_fading_speed, extra_forgetting):
    seqs, length, depth = layer_feed.shape
    columns = address_mapping.shape[1]
    heads = columns // HEAD
    pack = math.gcd(heads, 4)
    width = pack * HEAD
    quads = heads // pack
    rows = math.gcd(length, 4 * HEAD)
    per_seq = length // rows
    all_heads = beta_mapping_matrix.shape[1]
    speed = jnp.repeat(-jnp.exp(logged_fading_speed), HEAD)[None, :]
    whole = lambda shape: pl.BlockSpec(shape, lambda i: (0, 0), pipeline_mode=pl.Buffered(1))
    return pl.pallas_call(
        functools.partial(kernel, per_seq, pack),
        grid=(seqs * per_seq,),
        out_shape=jax.ShapeDtypeStruct((seqs, quads, 2 * HEAD, width), F32),
        in_specs=[
            pl.BlockSpec((rows, depth), lambda i: (i, 0)),
            whole((depth, columns)),
            whole((depth, columns)),
            whole((depth, all_heads)),
            whole((depth, all_heads)),
            whole((1, columns)),
            pl.BlockSpec((rows, heads), lambda i: (i, 0)),
        ],
        out_specs=pl.BlockSpec((1, quads, 2 * HEAD, width), lambda i: (i // per_seq, 0, 0, 0)),
        scratch_shapes=[
            pltpu.VMEM((depth, 128), BF16),
            pltpu.VMEM((quads, 2 * HEAD, width), F32),
        ],
        compiler_params=pltpu.CompilerParams(
            dimension_semantics=("arbitrary",), vmem_limit_bytes=56 * 2**20),
    )(layer_feed.reshape(seqs * length, depth), address_mapping, content_mapping,
      beta_mapping_matrix, forgetting_mapping, speed, extra_forgetting.reshape(seqs * length, heads))


def matmul(left, right):
    return jnp.einsum("shij,shjk->shik", left, right, precision=finest)


def suffix_product(part, axis):
    count = lax.axis_size(axis)
    ahead = count - 1 - lax.axis_index(axis)
    gathered = lax.all_gather(part, axis)
    start = jnp.broadcast_to(jnp.eye(HEAD, dtype=F32), part.shape)

    def one(hop, carry):
        return matmul(carry, lax.dynamic_index_in_dim(gathered, count - 1 - hop, 0, False))

    return lax.fori_loop(0, ahead, one, start)


def body(layer_feed, address_mapping, content_mapping, beta_mapping_matrix, forgetting_mapping,
         logged_fading_speed, extra_forgetting, opening_probe):
    seqs = layer_feed.shape[0]
    heads = address_mapping.shape[1] // HEAD
    maps = device_maps(layer_feed, address_mapping, content_mapping, beta_mapping_matrix,
                       forgetting_mapping, logged_fading_speed, extra_forgetting)
    quads, width = maps.shape[1], maps.shape[3]
    maps = maps.reshape(seqs, quads, 2, HEAD, width // HEAD, HEAD)
    maps = maps.transpose(2, 0, 1, 4, 5, 3).reshape(2, seqs, heads, HEAD, HEAD)
    offset, transfer = maps[0], maps[1]
    rows = HEAD // lax.axis_size("sp")
    first_row = lax.axis_index("sp") * rows
    terms = matmul(suffix_product(transfer, "sp"), offset)
    final = lax.psum_scatter(terms, "sp", scatter_dimension=2, tiled=True)
    query = opening_probe.reshape(seqs, heads, HEAD)
    query = lax.dynamic_slice_in_dim(query, first_row, rows, 2).astype(F32)
    read = lax.psum(jnp.einsum("shk,shkv->shv", query, final, precision=finest), "sp")
    read = read * lax.rsqrt(jnp.mean(read * read, axis=-1, keepdims=True) + 1e-06)
    return final.astype(BF16), read.reshape(seqs, heads * HEAD).astype(BF16)


def solution(mesh):
    in_specs = (
        P("grp", "sp", None),
        P(None, "tp"),
        P(None, "tp"),
        P(),
        P(),
        P("tp"),
        P("grp", "sp", "tp"),
        P("grp", "tp"),
    )
    out_specs = (P("grp", "tp", "sp", None), P("grp", "tp"))
    return jax.shard_map(body, mesh=mesh, in_specs=in_specs, out_specs=out_specs, check_vma=False)
```

```python
import functools
import math

import jax
import jax.numpy as jnp
from jax import lax
from jax.experimental import pallas as pl
from jax.experimental.pallas import tpu as pltpu
from jax.sharding import PartitionSpec as P

HEAD = 64
F32 = jnp.float32
BF16 = jnp.bfloat16

finest = lax.Precision.HIGHEST


def mm(left, right):
    return jnp.dot(left, right, preferred_element_type=F32)


def iota(shape, dim):
    return lax.broadcasted_iota(jnp.int32, shape, dim)


def onehot(flag):
    return jnp.where(flag, 1.0, 0.0).astype(BF16)


def lane_masks(pack, width):
    lane_head = iota((1, width), 1) // HEAD
    return [onehot(lane_head == h) for h in range(pack)]


def blockdiag(member, masks):
    return jnp.concatenate([member * mask for mask in masks], axis=0)


def split(member):
    high = member.astype(BF16)
    return high, (member - high.astype(F32)).astype(BF16)


def finish(masks, pack, sp, units, per, q_ref, ctx_ref, read_ref, maps, arrived, leaving,
           landed, reads, send_sem, recv_sem, send_out, recv_out):
    me = lax.axis_index("sp")
    rows = HEAD // sp
    width = pack * HEAD
    lines = width // 128
    eye = jnp.where(iota((HEAD, width), 0) == iota((HEAD, width), 1) % HEAD, 1.0, 0.0)
    head_row = iota((8, width), 0)
    head_lane = iota((8, width), 1) // HEAD
    for i in range(per):
        for d in range(1, sp):
            peer_copy(maps.at[0], arrived.at[lax.rem(me + sp - d, sp), i], send_sem.at[0],
                      recv_sem.at[i, d], me).wait_recv()
        final = arrived[0, i, :HEAD, :]
        for j in range(1, sp):
            high, low = split(final)
            t_high, t_low = split(arrived[j, i, HEAD:, :])
            t_high = blockdiag(t_high, masks)
            final = (mm(high, t_high) + mm(low, t_high) + mm(high, blockdiag(t_low, masks))
                     + arrived[j, i, :HEAD, :])
        query = jnp.where(head_row == head_lane, q_ref[me * per + i], 0.0)
        read = lax.dot_general(query, final, (((1,), (1,)), ((), ())), precision=finest,
                               preferred_element_type=F32)
        read = read * lax.rsqrt(jnp.mean(read * read, axis=1, keepdims=True) + 1e-06)
        read = jnp.dot(read, eye, precision=finest, preferred_element_type=F32)
        read = jnp.sum(jnp.where(head_row == head_lane, read, 0.0), axis=0, keepdims=True)
        turned = final.T
        for j in range(sp):
            for h in range(pack):
                leaving[i, j, h * rows:(h + 1) * rows, :HEAD] = (
                    turned[h * HEAD + j * rows:h * HEAD + (j + 1) * rows, :])
            for line in range(lines):
                leaving[i, j, pack * rows + line:pack * rows + line + 1, :] = (
                    read[:, line * 128:(line + 1) * 128])
        for d in range(1, sp):
            peer = lax.rem(me + d, sp)
            peer_copy(leaving.at[i, peer], landed.at[me * per + i], send_out.at[i, d],
                      recv_out.at[i, d], peer).start()
        landed[me * per + i] = leaving[i, me]
    for i in range(per):
        for d in range(1, sp):
            peer = lax.rem(me + sp - d, sp)
            peer_copy(leaving.at[i, 0], landed.at[peer * per + i], send_out.at[i, d],
                      recv_out.at[i, d], peer).wait_recv()
    quads = reads.shape[1] // width
    for u in range(units):
        ctx_ref[u] = landed[u, :pack * rows, :HEAD].astype(BF16)
        for line in range(lines):
            at = (u % quads) * width + line * 128
            reads[u // quads:u // quads + 1, at:at + 128] = (
                landed[u, pack * rows + line:pack * rows + line + 1, :])
    read_ref[...] = reads[...].astype(BF16)
    for i in range(per):
        for d in range(1, sp):
            peer = lax.rem(me + d, sp)
            peer_copy(leaving.at[i, peer], landed.at[me * per + i], send_out.at[i, d],
                      recv_out.at[i, d], peer).wait_send()
    for u in range(units):
        @pl.when(u // per != me)
        def _():
            peer_copy(maps.at[u], arrived.at[me, u % per], send_sem.at[u],
                      recv_sem.at[u % per, 0], u // per).wait_send()


def peer_copy(source, target, send_sem, recv_sem, peer):
    return pltpu.make_async_remote_copy(
        src_ref=source, dst_ref=target, send_sem=send_sem, recv_sem=recv_sem,
        device_id={"sp": peer}, device_id_type=pl.DeviceIdType.MESH)


def local_stage(step, steps_per_seq, pack, x_ref, wk_ref, wv_ref, wb_ref, wf_ref, speed_ref,
                extra_ref, gate_weight, state):
    rows = x_ref.shape[0]
    columns = wk_ref.shape[1]
    heads = columns // HEAD
    width = pack * HEAD
    quads = columns // width
    chunks = rows // HEAD
    all_heads = wb_ref.shape[0]
    first_head = lax.axis_index("tp") * heads
    masks = lane_masks(pack, width)

    row_c = iota((HEAD, width), 0)
    lane_c = iota((HEAD, width), 1) % HEAD
    below = row_c > lane_c
    diagonal = row_c == lane_c
    apart = row_c ^ lane_c

    @pl.when(step == 0)
    def _():
        source = iota((128, all_heads), 1)
        lane = iota((128, all_heads), 0)
        to_beta = onehot((source == first_head + lane) & (lane < heads))
        to_decay = onehot((source == first_head + lane - heads) & (lane >= heads) & (lane < 2 * heads))
        gate_weight[...] = (mm(to_beta, wb_ref[...]) + mm(to_decay, wf_ref[...])).astype(BF16)

    @pl.when(lax.rem(step, steps_per_seq) == 0)
    def _():
        eye = jnp.where(diagonal, 1.0, 0.0)
        for quad in range(quads):
            state[quad, :HEAD, :] = jnp.zeros((HEAD, width), F32)
            state[quad, HEAD:, :] = eye

    x = x_ref[...]
    gates = lax.dot_general(x, gate_weight[...], (((1,), (1,)), ((), ())),
                            preferred_element_type=F32).astype(BF16)
    key_proj = mm(x, wk_ref[...]).astype(BF16).astype(F32)
    value_proj = mm(x, wv_ref[...]).astype(BF16).astype(F32)

    source = iota((128, columns), 0)
    target = iota((128, columns), 1) // HEAD
    beta_pre = mm(gates, onehot(source == target))
    decay_pre = mm(gates, onehot(source == target + heads))
    source = iota((heads, columns), 0)
    target = iota((heads, columns), 1) // HEAD
    extra = mm(extra_ref[...], onehot(source == target))

    beta = jax.nn.sigmoid(beta_pre)
    softplus = jnp.maximum(decay_pre, 0.0) + jnp.log1p(jnp.exp(-jnp.abs(decay_pre)))
    speed = jnp.dot(-jnp.exp(speed_ref[...]), jnp.where(source == target, 1.0, 0.0),
                    precision=finest, preferred_element_type=F32)
    gamma = speed * softplus + extra
    high = gamma.astype(BF16)
    rest = gamma - high.astype(F32)
    middle = rest.astype(BF16)
    low = (rest - middle.astype(F32)).astype(BF16)
    r_idx = iota((rows, rows), 0)
    c_idx = iota((rows, rows), 1)
    running = onehot((r_idx >= c_idx) & (r_idx // HEAD == c_idx // HEAD))
    cumul = mm(running, high) + mm(running, middle) + mm(running, low)

    key = key_proj * jax.nn.sigmoid(key_proj)
    value = value_proj * jax.nn.sigmoid(value_proj)
    group = onehot(iota((width, width), 0) // HEAD == iota((width, width), 1) // HEAD)
    squares = (key * key).astype(BF16)
    total = jnp.concatenate(
        [mm(squares[:, q * width:(q + 1) * width], group) for q in range(quads)], axis=1)
    key = key * lax.rsqrt(total + 1e-06)

    units = []
    for chunk in range(chunks):
        for quad in range(quads):
            units.append((slice(chunk * HEAD, (chunk + 1) * HEAD), slice(quad * width, (quad + 1) * width)))

    lowers = []
    for rs, cs in units:
        k16 = key[rs, cs].astype(BF16)
        gram = lax.dot_general(k16, blockdiag(k16, masks), (((1,), (1,)), ((), ())),
                               preferred_element_type=F32)
        cum = cumul[rs, cs]
        across = jnp.sum(jnp.where(diagonal, cum, 0.0), axis=0, keepdims=True)
        weights = jnp.exp(jnp.where(below, cum - across, 0.0))
        lowers.append(jnp.where(below, beta[rs, cs] * gram * weights, 0.0))

    inverses = [jnp.where(diagonal, 1.0, jnp.where(apart == 1, -lower, 0.0)) for lower in lowers]
    size = 2
    while size < HEAD:
        inv16 = [inverse.astype(BF16) for inverse in inverses]
        parts = []
        for lower, inverse in zip(lowers, inv16):
            corner = jnp.where((apart >= size) & (apart < 2 * size), lower, 0.0).astype(BF16)
            parts.append(mm(inverse, blockdiag(corner, masks)).astype(BF16))
        inverses = [inverse - mm(part, blockdiag(i16, masks))
                    for inverse, part, i16 in zip(inverses, parts, inv16)]
        size *= 2

    maps = []
    for (rs, cs), inverse in zip(units, inverses):
        i16 = inverse.astype(BF16)
        b, k, cum = beta[rs, cs], key[rs, cs], cumul[rs, cs]
        update = mm(i16, blockdiag((b * value[rs, cs]).astype(BF16), masks))
        mixing = mm(i16, blockdiag((b * jnp.exp(cum) * k).astype(BF16), masks))
        last = cum[HEAD - 1:HEAD, :]
        carried = (k * jnp.exp(last - cum)).astype(BF16)
        contract = (((0,), (0,)), ((), ()))
        offset = lax.dot_general(update.astype(BF16), carried, contract, preferred_element_type=F32)
        erase = lax.dot_general(mixing.astype(BF16), carried, contract, preferred_element_type=F32)
        offset = sum(offset[h * HEAD:(h + 1) * HEAD] * masks[h].astype(F32) for h in range(pack))
        erase = jnp.concatenate(
            [erase[h * HEAD:(h + 1) * HEAD].astype(BF16) * masks[h] for h in range(pack)], axis=0)
        maps.append((jnp.exp(last), erase, offset))

    for quad in range(quads):
        held = state[quad]
        for chunk in range(chunks):
            closing, erase, offset = maps[chunk * quads + quad]
            held = closing * held - mm(held.astype(BF16), erase)
            held = jnp.concatenate([held[:HEAD] + offset, held[HEAD:]], axis=0)
        state[quad] = held

def local_kernel(steps_per_seq, pack, x_ref, wk_ref, wv_ref, wb_ref, wf_ref, speed_ref, extra_ref,
                 out_ref, gate_weight, state):
    step = pl.program_id(0)
    local_stage(step, steps_per_seq, pack, x_ref, wk_ref, wv_ref, wb_ref, wf_ref, speed_ref, extra_ref,
                gate_weight, state)

    @pl.when(lax.rem(step, steps_per_seq) == steps_per_seq - 1)
    def _():
        out_ref[0] = state[...]


def kernel(steps_per_seq, pack, sp, x_ref, wk_ref, wv_ref, wb_ref, wf_ref, speed_ref, extra_ref,
           q_ref, ctx_ref, read_ref, gate_weight, state, maps, arrived, leaving, landed, reads,
           send_sem, recv_sem, send_out, recv_out):
    step = pl.program_id(0)
    steps = pl.num_programs(0)
    me = lax.axis_index("sp")
    width = pack * HEAD
    quads = state.shape[0]
    masks = lane_masks(pack, width)

    @pl.when(step == 0)
    def _():
        barrier = pltpu.get_barrier_semaphore()
        for d in range(1, sp):
            pl.semaphore_signal(barrier, inc=1, device_id={"sp": lax.rem(me + d, sp)},
                                device_id_type=pl.DeviceIdType.MESH)

    local_stage(step, steps_per_seq, pack, x_ref, wk_ref, wv_ref, wb_ref, wf_ref, speed_ref, extra_ref,
                gate_weight, state)
    units_all = maps.shape[0]
    per = units_all // sp

    @pl.when(step == steps_per_seq - 1)
    def _():
        pl.semaphore_wait(pltpu.get_barrier_semaphore(), sp - 1)

    @pl.when(lax.rem(step, steps_per_seq) == steps_per_seq - 1)
    def _():
        seqs = units_all // quads
        seq = lax.rem(step // steps_per_seq + me * per // quads + 1, seqs)
        for quad in range(quads):
            unit = seq * quads + quad
            owner = unit // per
            slot = lax.rem(unit, per)

            @pl.when(owner != me)
            def _():
                maps[unit] = state[quad]
                away = lax.rem(owner - me + sp, sp)
                peer_copy(maps.at[unit], arrived.at[me, slot], send_sem.at[unit],
                          recv_sem.at[slot, away], owner).start()

            @pl.when(owner == me)
            def _():
                arrived[me, slot] = state[quad]

    @pl.when(step == steps - 1)
    def _():
        finish(masks, pack, sp, units_all, per, q_ref, ctx_ref, read_ref, maps, arrived,
               leaving, landed, reads, send_sem, recv_sem, send_out, recv_out)


def fused(layer_feed, address_mapping, content_mapping, beta_mapping_matrix, forgetting_mapping,
          logged_fading_speed, extra_forgetting, opening_probe):
    seqs, length, depth = layer_feed.shape
    columns = address_mapping.shape[1]
    heads = columns // HEAD
    pack = math.gcd(heads, 4)
    width = pack * HEAD
    quads = heads // pack
    units = seqs * quads
    sp = lax.axis_size("sp")
    per = units // sp
    rows = math.gcd(length, 4 * HEAD)
    per_seq = length // rows
    steps = seqs * per_seq
    all_heads = beta_mapping_matrix.shape[1]
    own_rows = HEAD // sp
    tall = -(-(pack * own_rows + width // 128) // 8) * 8
    whole = lambda shape: pl.BlockSpec(shape, lambda i: (0,) * len(shape), pipeline_mode=pl.Buffered(1))

    def turn(i):
        own = lax.axis_index("sp") * per // quads
        return (lax.rem(i + (own + 1) * per_seq, steps), 0)

    context, read = pl.pallas_call(
        functools.partial(kernel, per_seq, pack, sp),
        grid=(steps,),
        out_shape=(jax.ShapeDtypeStruct((units, pack * own_rows, HEAD), BF16),
                   jax.ShapeDtypeStruct((seqs, columns), BF16)),
        in_specs=[
            pl.BlockSpec((rows, depth), turn),
            whole((depth, columns)),
            whole((depth, columns)),
            whole((all_heads, depth)),
            whole((all_heads, depth)),
            whole((1, heads)),
            pl.BlockSpec((rows, heads), turn),
            whole((units, 1, width)),
        ],
        out_specs=(pl.BlockSpec((units, pack * own_rows, HEAD), lambda i: (0, 0, 0)),
                   pl.BlockSpec((seqs, columns), lambda i: (0, 0))),
        scratch_shapes=[
            pltpu.VMEM((128, depth), BF16),
            pltpu.VMEM((quads, 2 * HEAD, width), F32),
            pltpu.VMEM((units, 2 * HEAD, width), F32),
            pltpu.VMEM((sp, per, 2 * HEAD, width), F32),
            pltpu.VMEM((per, sp, tall, 128), F32),
            pltpu.VMEM((units, tall, 128), F32),
            pltpu.VMEM((seqs, columns), F32),
            pltpu.SemaphoreType.DMA((units,)),
            pltpu.SemaphoreType.DMA((per, sp)),
            pltpu.SemaphoreType.DMA((per, sp)),
            pltpu.SemaphoreType.DMA((per, sp)),
        ],
        compiler_params=pltpu.CompilerParams(
            dimension_semantics=("arbitrary",), vmem_limit_bytes=56 * 2**20,
            collective_id=0, has_side_effects=True),
    )(layer_feed.reshape(seqs * length, depth), address_mapping, content_mapping,
      beta_mapping_matrix.T, forgetting_mapping.T, logged_fading_speed[None, :],
      extra_forgetting.reshape(seqs * length, heads),
      opening_probe.reshape(units, 1, width).astype(F32))
    return context.reshape(seqs, heads, own_rows, HEAD), read


def device_maps(layer_feed, address_mapping, content_mapping, beta_mapping_matrix,
                forgetting_mapping, logged_fading_speed, extra_forgetting):
    seqs, length, depth = layer_feed.shape
    columns = address_mapping.shape[1]
    heads = columns // HEAD
    pack = math.gcd(heads, 4)
    width = pack * HEAD
    quads = heads // pack
    rows = math.gcd(length, 4 * HEAD)
    per_seq = length // rows
    all_heads = beta_mapping_matrix.shape[1]
    whole = lambda shape: pl.BlockSpec(shape, lambda i: (0, 0), pipeline_mode=pl.Buffered(1))
    return pl.pallas_call(
        functools.partial(local_kernel, per_seq, pack),
        grid=(seqs * per_seq,),
        out_shape=jax.ShapeDtypeStruct((seqs, quads, 2 * HEAD, width), F32),
        in_specs=[
            pl.BlockSpec((rows, depth), lambda i: (i, 0)),
            whole((depth, columns)),
            whole((depth, columns)),
            whole((all_heads, depth)),
            whole((all_heads, depth)),
            whole((1, heads)),
            pl.BlockSpec((rows, heads), lambda i: (i, 0)),
        ],
        out_specs=pl.BlockSpec((1, quads, 2 * HEAD, width), lambda i: (i // per_seq, 0, 0, 0)),
        scratch_shapes=[
            pltpu.VMEM((128, depth), BF16),
            pltpu.VMEM((quads, 2 * HEAD, width), F32),
        ],
        compiler_params=pltpu.CompilerParams(
            dimension_semantics=("arbitrary",), vmem_limit_bytes=56 * 2**20),
    )(layer_feed.reshape(seqs * length, depth), address_mapping, content_mapping,
      beta_mapping_matrix.T, forgetting_mapping.T, logged_fading_speed[None, :], extra_forgetting.reshape(seqs * length, heads))


def matmul(left, right):
    return jnp.einsum("shij,shjk->shik", left, right, precision=finest)


def suffix_product(part, axis):
    count = lax.axis_size(axis)
    ahead = count - 1 - lax.axis_index(axis)
    gathered = lax.all_gather(part, axis)
    start = jnp.broadcast_to(jnp.eye(HEAD, dtype=F32), part.shape)

    def one(hop, carry):
        return matmul(carry, lax.dynamic_index_in_dim(gathered, count - 1 - hop, 0, False))

    return lax.fori_loop(0, ahead, one, start)


def body(layer_feed, address_mapping, content_mapping, beta_mapping_matrix, forgetting_mapping,
         logged_fading_speed, extra_forgetting, opening_probe):
    seqs = layer_feed.shape[0]
    heads = address_mapping.shape[1] // HEAD
    sp = lax.axis_size("sp")
    pack = math.gcd(heads, 4)
    if pack > 1 and (seqs * heads // pack) % sp == 0 and HEAD % (8 * sp) == 0:
        return fused(layer_feed, address_mapping, content_mapping, beta_mapping_matrix,
                     forgetting_mapping, logged_fading_speed, extra_forgetting, opening_probe)
    maps = device_maps(layer_feed, address_mapping, content_mapping, beta_mapping_matrix,
                       forgetting_mapping, logged_fading_speed, extra_forgetting)
    quads, width = maps.shape[1], maps.shape[3]
    maps = maps.reshape(seqs, quads, 2, HEAD, width // HEAD, HEAD)
    maps = maps.transpose(2, 0, 1, 4, 5, 3).reshape(2, seqs, heads, HEAD, HEAD)
    offset, transfer = maps[0], maps[1]
    rows = HEAD // lax.axis_size("sp")
    first_row = lax.axis_index("sp") * rows
    terms = matmul(suffix_product(transfer, "sp"), offset)
    final = lax.psum_scatter(terms, "sp", scatter_dimension=2, tiled=True)
    query = opening_probe.reshape(seqs, heads, HEAD)
    query = lax.dynamic_slice_in_dim(query, first_row, rows, 2).astype(F32)
    read = lax.psum(jnp.einsum("shk,shkv->shv", query, final, precision=finest), "sp")
    read = read * lax.rsqrt(jnp.mean(read * read, axis=-1, keepdims=True) + 1e-06)
    return final.astype(BF16), read.reshape(seqs, heads * HEAD).astype(BF16)


def solution(mesh):
    in_specs = (
        P("grp", "sp", None),
        P(None, "tp"),
        P(None, "tp"),
        P(),
        P(),
        P("tp"),
        P("grp", "sp", "tp"),
        P("grp", "tp"),
    )
    out_specs = (P("grp", "tp", "sp", None), P("grp", "tp"))
    return jax.shard_map(body, mesh=mesh, in_specs=in_specs, out_specs=out_specs, check_vma=False)
```

```python
import functools
import math

import jax
import jax.numpy as jnp
from jax import lax
from jax.experimental import pallas as pl
from jax.experimental.pallas import tpu as pltpu
from jax.sharding import PartitionSpec as P

HEAD = 64
F32 = jnp.float32
BF16 = jnp.bfloat16

finest = lax.Precision.HIGHEST


def mm(left, right):
    return jnp.dot(left, right, preferred_element_type=F32)


def iota(shape, dim):
    return lax.broadcasted_iota(jnp.int32, shape, dim)


def onehot(flag):
    return jnp.where(flag, 1.0, 0.0).astype(BF16)


def lane_masks(pack, width):
    tile = min(128, width)
    lane_head = iota((1, tile), 1) // HEAD
    return [onehot(lane_head == h) for h in range(tile // HEAD)]


def blockdiag(member, masks):
    width = member.shape[1]
    tile = masks[0].shape[1]
    zeros = jnp.zeros((member.shape[0], tile), member.dtype)
    lines = []
    for head in range(width // HEAD):
        place = head * HEAD // tile
        pieces = [zeros] * (width // tile)
        pieces[place] = member[:, place * tile:(place + 1) * tile] * masks[head % len(masks)]
        lines.append(jnp.concatenate(pieces, axis=1))
    return jnp.concatenate(lines, axis=0)


def split(member):
    high = member.astype(BF16)
    return high, (member - high.astype(F32)).astype(BF16)


def finish(masks, pack, sp, units, per, q_ref, ctx_ref, read_ref, maps, arrived, leaving,
           landed, reads, send_sem, recv_sem, send_out, recv_out):
    me = lax.axis_index("sp")
    rows = HEAD // sp
    width = pack * HEAD
    lines = width // 128
    eye = jnp.where(iota((HEAD, width), 0) == iota((HEAD, width), 1) % HEAD, 1.0, 0.0)
    quads = reads.shape[1] // width
    probe = q_ref[...].astype(F32)
    head_row = iota((8, width), 0)
    head_lane = iota((8, width), 1) // HEAD
    for i in range(per):
        for d in range(1, sp):
            peer_copy(maps.at[0], arrived.at[lax.rem(me + sp - d, sp), i], send_sem.at[0],
                      recv_sem.at[i, d], me).wait_recv()
        final = arrived[0, i, :HEAD, :]
        for j in range(1, sp):
            high, low = split(final)
            t_high, t_low = split(arrived[j, i, HEAD:, :])
            t_high = blockdiag(t_high, masks)
            final = (mm(high, t_high) + mm(low, t_high) + mm(high, blockdiag(t_low, masks))
                     + arrived[j, i, :HEAD, :])
        query = jnp.zeros((1, width), F32)
        for u in range(i, units, per):
            mine = jnp.where(u == me * per + i, 1.0, 0.0)
            at = (u % quads) * width
            query = query + mine * probe[u // quads:u // quads + 1, at:at + width]
        query = jnp.where(head_row == head_lane, query, 0.0)
        read = lax.dot_general(query, final, (((1,), (1,)), ((), ())), precision=finest,
                               preferred_element_type=F32)
        read = read * lax.rsqrt(jnp.mean(read * read, axis=1, keepdims=True) + 1e-06)
        read = jnp.dot(read, eye, precision=finest, preferred_element_type=F32)
        read = jnp.sum(jnp.where(head_row == head_lane, read, 0.0), axis=0, keepdims=True)
        turned = final.T
        for j in range(sp):
            for h in range(pack):
                leaving[i, j, h * rows:(h + 1) * rows, :HEAD] = (
                    turned[h * HEAD + j * rows:h * HEAD + (j + 1) * rows, :])
            for line in range(lines):
                leaving[i, j, pack * rows + line:pack * rows + line + 1, :] = (
                    read[:, line * 128:(line + 1) * 128])
        for d in range(1, sp):
            peer = lax.rem(me + d, sp)
            peer_copy(leaving.at[i, peer], landed.at[me * per + i], send_out.at[i, d],
                      recv_out.at[i, d], peer).start()
        landed[me * per + i] = leaving[i, me]
    for i in range(per):
        for d in range(1, sp):
            peer = lax.rem(me + sp - d, sp)
            peer_copy(leaving.at[i, 0], landed.at[peer * per + i], send_out.at[i, d],
                      recv_out.at[i, d], peer).wait_recv()
    for u in range(units):
        ctx_ref[u] = landed[u, :pack * rows, :HEAD].astype(BF16)
        for line in range(lines):
            at = (u % quads) * width + line * 128
            reads[u // quads:u // quads + 1, at:at + 128] = (
                landed[u, pack * rows + line:pack * rows + line + 1, :])
    read_ref[...] = reads[...].astype(BF16)
    for i in range(per):
        for d in range(1, sp):
            peer = lax.rem(me + d, sp)
            peer_copy(leaving.at[i, peer], landed.at[me * per + i], send_out.at[i, d],
                      recv_out.at[i, d], peer).wait_send()
    for u in range(units):
        @pl.when(u // per != me)
        def _():
            peer_copy(maps.at[u], arrived.at[me, u % per], send_sem.at[u],
                      recv_sem.at[u % per, 0], u // per).wait_send()


def peer_copy(source, target, send_sem, recv_sem, peer):
    return pltpu.make_async_remote_copy(
        src_ref=source, dst_ref=target, send_sem=send_sem, recv_sem=recv_sem,
        device_id={"sp": peer}, device_id_type=pl.DeviceIdType.MESH)


def local_stage(step, steps_per_seq, pack, x_ref, wk_ref, wv_ref, wb_ref, wf_ref, speed_ref,
                extra_ref, gate_weight, state):
    rows = x_ref.shape[0]
    columns = wk_ref.shape[1]
    heads = columns // HEAD
    width = pack * HEAD
    quads = columns // width
    chunks = rows // HEAD
    all_heads = wb_ref.shape[0]
    first_head = lax.axis_index("tp") * heads
    masks = lane_masks(pack, width)

    row_c = iota((HEAD, width), 0)
    lane_c = iota((HEAD, width), 1) % HEAD
    below = row_c > lane_c
    diagonal = row_c == lane_c
    apart = row_c ^ lane_c

    @pl.when(step == 0)
    def _():
        source = iota((128, all_heads), 1)
        lane = iota((128, all_heads), 0)
        to_beta = onehot((source == first_head + lane) & (lane < heads))
        to_decay = onehot((source == first_head + lane - heads) & (lane >= heads) & (lane < 2 * heads))
        gate_weight[...] = (mm(to_beta, wb_ref[...]) + mm(to_decay, wf_ref[...])).astype(BF16)

    @pl.when(lax.rem(step, steps_per_seq) == 0)
    def _():
        eye = jnp.where(diagonal, 1.0, 0.0)
        for quad in range(quads):
            state[quad, :HEAD, :] = jnp.zeros((HEAD, width), F32)
            state[quad, HEAD:, :] = eye

    x = x_ref[...]
    gates = lax.dot_general(x, gate_weight[...], (((1,), (1,)), ((), ())),
                            preferred_element_type=F32).astype(BF16)
    key_proj = mm(x, wk_ref[...]).astype(BF16).astype(F32)
    value_proj = mm(x, wv_ref[...]).astype(BF16).astype(F32)

    source = iota((128, columns), 0)
    target = iota((128, columns), 1) // HEAD
    beta_pre = mm(gates, onehot(source == target))
    decay_pre = mm(gates, onehot(source == target + heads))
    source = iota((heads, columns), 0)
    target = iota((heads, columns), 1) // HEAD
    extra = lax.dot_general(extra_ref[0], onehot(source == target), (((0,), (0,)), ((), ())),
                            preferred_element_type=F32)

    beta = jax.nn.sigmoid(beta_pre)
    softplus = jnp.maximum(decay_pre, 0.0) + jnp.log1p(jnp.exp(-jnp.abs(decay_pre)))
    speed = jnp.dot(-jnp.exp(speed_ref[...]), jnp.where(source == target, 1.0, 0.0),
                    precision=finest, preferred_element_type=F32)
    gamma = speed * softplus + extra
    high = gamma.astype(BF16)
    rest = gamma - high.astype(F32)
    middle = rest.astype(BF16)
    low = (rest - middle.astype(F32)).astype(BF16)
    r_idx = iota((rows, rows), 0)
    c_idx = iota((rows, rows), 1)
    running = onehot((r_idx >= c_idx) & (r_idx // HEAD == c_idx // HEAD))
    cumul = mm(running, high) + mm(running, middle) + mm(running, low)

    key = key_proj * jax.nn.sigmoid(key_proj)
    value = value_proj * jax.nn.sigmoid(value_proj)
    group = onehot(iota((width, width), 0) // HEAD == iota((width, width), 1) // HEAD)
    squares = (key * key).astype(BF16)
    total = jnp.concatenate(
        [mm(squares[:, q * width:(q + 1) * width], group) for q in range(quads)], axis=1)
    key = key * lax.rsqrt(total + 1e-06)

    units = []
    for chunk in range(chunks):
        for quad in range(quads):
            units.append((slice(chunk * HEAD, (chunk + 1) * HEAD), slice(quad * width, (quad + 1) * width)))

    grown = jnp.exp(cumul)
    key16 = key.astype(BF16)
    weighted_key = (beta * grown * key).astype(BF16)
    weighted_value = (beta * value).astype(BF16)
    tile = masks[0].shape[1]
    eye16 = onehot(diagonal)
    levels = [onehot((apart >= 1 << p) & (apart < 2 << p)) for p in range(HEAD.bit_length() - 1)]
    contract = (((0,), (0,)), ((), ()))

    grams = []
    for rs, cs in units:
        grams.append(lax.dot_general(key16[rs, cs], blockdiag(key16[rs, cs], masks),
                                     (((1,), (1,)), ((), ())), preferred_element_type=F32))
    lowers = []
    for (rs, cs), gram in zip(units, grams):
        cum = cumul[rs, cs]
        across = jnp.sum(jnp.where(diagonal, cum, 0.0), axis=0, keepdims=True)
        weights = jnp.exp(jnp.where(below, cum - across, -1e30))
        lowers.append((beta[rs, cs] * gram * weights).astype(BF16))

    inverses = [eye16 - lower * levels[0] for lower in lowers]
    for level in levels[1:]:
        parts = [mm(inverse, blockdiag(lower * level, masks)).astype(BF16)
                 for lower, inverse in zip(lowers, inverses)]
        inverses = [inverse - mm(part, blockdiag(inverse, masks)).astype(BF16)
                    for inverse, part in zip(inverses, parts)]

    updates = [mm(inverse, blockdiag(weighted_value[rs, cs], masks)).astype(BF16)
               for (rs, cs), inverse in zip(units, inverses)]
    mixings = [mm(inverse, blockdiag(weighted_key[rs, cs], masks)).astype(BF16)
               for (rs, cs), inverse in zip(units, inverses)]
    closings, erases, offsets = [], [], []
    upper_lanes = iota((HEAD, tile), 1) >= HEAD
    for (rs, cs), update, mixing in zip(units, updates, mixings):
        last = cumul[rs, cs][HEAD - 1:HEAD, :]
        carried = (key[rs, cs] * jnp.exp(last - cumul[rs, cs])).astype(BF16)
        closings.append(jnp.exp(last))
        offset_tiles, erase_lines = [], []
        zeros = jnp.zeros((tile, tile), BF16)
        for place in range(width // tile):
            ts = slice(place * tile, (place + 1) * tile)
            offset = lax.dot_general(update[:, ts], carried[:, ts], contract, preferred_element_type=F32)
            erase = lax.dot_general(mixing[:, ts], carried[:, ts], contract, preferred_element_type=F32)
            if tile > HEAD:
                offset = jnp.where(upper_lanes, offset[HEAD:], offset[:HEAD])
            offset_tiles.append(offset)
            erase = erase.astype(BF16)
            erase = jnp.concatenate(
                [erase[h * HEAD:(h + 1) * HEAD] * masks[h] for h in range(tile // HEAD)], axis=0)
            line = [zeros] * (width // tile)
            line[place] = erase
            erase_lines.append(jnp.concatenate(line, axis=1))
        offsets.append(jnp.concatenate(offset_tiles, axis=1))
        erases.append(jnp.concatenate(erase_lines, axis=0))

    held = [(state[quad, :HEAD, :], state[quad, HEAD:, :]) for quad in range(quads)]
    for chunk in range(chunks):
        for quad in range(quads):
            u = chunk * quads + quad
            above, under = held[quad]
            erased = mm(jnp.concatenate([above, under], axis=0).astype(BF16), erases[u])
            held[quad] = (closings[u] * above - erased[:HEAD] + offsets[u],
                          closings[u] * under - erased[HEAD:])
    for quad in range(quads):
        state[quad, :HEAD, :], state[quad, HEAD:, :] = held[quad]


def local_kernel(steps_per_seq, pack, x_ref, wk_ref, wv_ref, wb_ref, wf_ref, speed_ref, extra_ref,
                 out_ref, gate_weight, state):
    step = pl.program_id(0)
    local_stage(step, steps_per_seq, pack, x_ref, wk_ref, wv_ref, wb_ref, wf_ref, speed_ref, extra_ref,
                gate_weight, state)

    @pl.when(lax.rem(step, steps_per_seq) == steps_per_seq - 1)
    def _():
        out_ref[0] = state[...]


def kernel(steps_per_seq, pack, sp, x_ref, wk_ref, wv_ref, wb_ref, wf_ref, speed_ref, extra_ref,
           q_ref, ctx_ref, read_ref, gate_weight, state, maps, arrived, leaving, landed, reads,
           send_sem, recv_sem, send_out, recv_out):
    step = pl.program_id(0)
    steps = pl.num_programs(0)
    me = lax.axis_index("sp")
    width = pack * HEAD
    quads = state.shape[0]
    masks = lane_masks(pack, width)

    @pl.when(step == 0)
    def _():
        barrier = pltpu.get_barrier_semaphore()
        for d in range(1, sp):
            pl.semaphore_signal(barrier, inc=1, device_id={"sp": lax.rem(me + d, sp)},
                                device_id_type=pl.DeviceIdType.MESH)

    local_stage(step, steps_per_seq, pack, x_ref, wk_ref, wv_ref, wb_ref, wf_ref, speed_ref, extra_ref,
                gate_weight, state)
    units_all = maps.shape[0]
    per = units_all // sp

    @pl.when(step == steps_per_seq - 1)
    def _():
        pl.semaphore_wait(pltpu.get_barrier_semaphore(), sp - 1)

    @pl.when(lax.rem(step, steps_per_seq) == steps_per_seq - 1)
    def _():
        seqs = units_all // quads
        seq = lax.rem(step // steps_per_seq + me * per // quads + 1, seqs)
        for quad in range(quads):
            unit = seq * quads + quad
            owner = unit // per
            slot = lax.rem(unit, per)

            @pl.when(owner != me)
            def _():
                maps[unit] = state[quad]
                away = lax.rem(owner - me + sp, sp)
                peer_copy(maps.at[unit], arrived.at[me, slot], send_sem.at[unit],
                          recv_sem.at[slot, away], owner).start()

            @pl.when(owner == me)
            def _():
                arrived[me, slot] = state[quad]

    @pl.when(step == steps - 1)
    def _():
        finish(masks, pack, sp, units_all, per, q_ref, ctx_ref, read_ref, maps, arrived,
               leaving, landed, reads, send_sem, recv_sem, send_out, recv_out)


def fused(layer_feed, address_mapping, content_mapping, beta_mapping_matrix, forgetting_mapping,
          logged_fading_speed, extra_forgetting, opening_probe):
    seqs, length, depth = layer_feed.shape
    columns = address_mapping.shape[1]
    heads = columns // HEAD
    pack = math.gcd(heads, 4)
    width = pack * HEAD
    quads = heads // pack
    units = seqs * quads
    sp = lax.axis_size("sp")
    per = units // sp
    rows = math.gcd(length, 4 * HEAD)
    per_seq = length // rows
    steps = seqs * per_seq
    all_heads = beta_mapping_matrix.shape[1]
    own_rows = HEAD // sp
    tall = -(-(pack * own_rows + width // 128) // 8) * 8
    whole = lambda shape: pl.BlockSpec(shape, lambda i: (0,) * len(shape), pipeline_mode=pl.Buffered(1))

    def turn(i):
        own = lax.axis_index("sp") * per // quads
        return (lax.rem(i + (own + 1) * per_seq, steps), 0)

    def turn_extra(i):
        block = turn(i)[0]
        return (block // per_seq, 0, lax.rem(block, per_seq))

    context, read = pl.pallas_call(
        functools.partial(kernel, per_seq, pack, sp),
        grid=(steps,),
        out_shape=(jax.ShapeDtypeStruct((units, pack * own_rows, HEAD), BF16),
                   jax.ShapeDtypeStruct((seqs, columns), BF16)),
        in_specs=[
            pl.BlockSpec((rows, depth), turn),
            whole((depth, columns)),
            whole((depth, columns)),
            whole((all_heads, depth)),
            whole((all_heads, depth)),
            whole((1, heads)),
            pl.BlockSpec((1, heads, rows), turn_extra),
            whole((seqs, columns)),
        ],
        out_specs=(pl.BlockSpec((units, pack * own_rows, HEAD), lambda i: (0, 0, 0)),
                   pl.BlockSpec((seqs, columns), lambda i: (0, 0))),
        scratch_shapes=[
            pltpu.VMEM((128, depth), BF16),
            pltpu.VMEM((quads, 2 * HEAD, width), F32),
            pltpu.VMEM((units, 2 * HEAD, width), F32),
            pltpu.VMEM((sp, per, 2 * HEAD, width), F32),
            pltpu.VMEM((per, sp, tall, 128), F32),
            pltpu.VMEM((units, tall, 128), F32),
            pltpu.VMEM((seqs, columns), F32),
            pltpu.SemaphoreType.DMA((units,)),
            pltpu.SemaphoreType.DMA((per, sp)),
            pltpu.SemaphoreType.DMA((per, sp)),
            pltpu.SemaphoreType.DMA((per, sp)),
        ],
        compiler_params=pltpu.CompilerParams(
            dimension_semantics=("arbitrary",), vmem_limit_bytes=56 * 2**20,
            collective_id=0, has_side_effects=True),
    )(layer_feed.reshape(seqs * length, depth), address_mapping, content_mapping,
      beta_mapping_matrix.T, forgetting_mapping.T, logged_fading_speed[None, :],
      extra_forgetting.transpose(0, 2, 1),
      opening_probe)
    return context.reshape(seqs, heads, own_rows, HEAD), read


def device_maps(layer_feed, address_mapping, content_mapping, beta_mapping_matrix,
                forgetting_mapping, logged_fading_speed, extra_forgetting):
    seqs, length, depth = layer_feed.shape
    columns = address_mapping.shape[1]
    heads = columns // HEAD
    pack = math.gcd(heads, 4)
    width = pack * HEAD
    quads = heads // pack
    rows = math.gcd(length, 4 * HEAD)
    per_seq = length // rows
    all_heads = beta_mapping_matrix.shape[1]
    whole = lambda shape: pl.BlockSpec(shape, lambda i: (0, 0), pipeline_mode=pl.Buffered(1))
    return pl.pallas_call(
        functools.partial(local_kernel, per_seq, pack),
        grid=(seqs * per_seq,),
        out_shape=jax.ShapeDtypeStruct((seqs, quads, 2 * HEAD, width), F32),
        in_specs=[
            pl.BlockSpec((rows, depth), lambda i: (i, 0)),
            whole((depth, columns)),
            whole((depth, columns)),
            whole((all_heads, depth)),
            whole((all_heads, depth)),
            whole((1, heads)),
            pl.BlockSpec((1, heads, rows), lambda i: (i // per_seq, 0, i % per_seq)),
        ],
        out_specs=pl.BlockSpec((1, quads, 2 * HEAD, width), lambda i: (i // per_seq, 0, 0, 0)),
        scratch_shapes=[
            pltpu.VMEM((128, depth), BF16),
            pltpu.VMEM((quads, 2 * HEAD, width), F32),
        ],
        compiler_params=pltpu.CompilerParams(
            dimension_semantics=("arbitrary",), vmem_limit_bytes=56 * 2**20),
    )(layer_feed.reshape(seqs * length, depth), address_mapping, content_mapping,
      beta_mapping_matrix.T, forgetting_mapping.T, logged_fading_speed[None, :], extra_forgetting.transpose(0, 2, 1))


def matmul(left, right):
    return jnp.einsum("shij,shjk->shik", left, right, precision=finest)


def suffix_product(part, axis):
    count = lax.axis_size(axis)
    ahead = count - 1 - lax.axis_index(axis)
    gathered = lax.all_gather(part, axis)
    start = jnp.broadcast_to(jnp.eye(HEAD, dtype=F32), part.shape)

    def one(hop, carry):
        return matmul(carry, lax.dynamic_index_in_dim(gathered, count - 1 - hop, 0, False))

    return lax.fori_loop(0, ahead, one, start)


def body(layer_feed, address_mapping, content_mapping, beta_mapping_matrix, forgetting_mapping,
         logged_fading_speed, extra_forgetting, opening_probe):
    seqs = layer_feed.shape[0]
    heads = address_mapping.shape[1] // HEAD
    sp = lax.axis_size("sp")
    pack = math.gcd(heads, 4)
    if pack > 1 and (seqs * heads // pack) % sp == 0 and HEAD % (8 * sp) == 0:
        return fused(layer_feed, address_mapping, content_mapping, beta_mapping_matrix,
                     forgetting_mapping, logged_fading_speed, extra_forgetting, opening_probe)
    maps = device_maps(layer_feed, address_mapping, content_mapping, beta_mapping_matrix,
                       forgetting_mapping, logged_fading_speed, extra_forgetting)
    quads, width = maps.shape[1], maps.shape[3]
    maps = maps.reshape(seqs, quads, 2, HEAD, width // HEAD, HEAD)
    maps = maps.transpose(2, 0, 1, 4, 5, 3).reshape(2, seqs, heads, HEAD, HEAD)
    offset, transfer = maps[0], maps[1]
    rows = HEAD // lax.axis_size("sp")
    first_row = lax.axis_index("sp") * rows
    terms = matmul(suffix_product(transfer, "sp"), offset)
    final = lax.psum_scatter(terms, "sp", scatter_dimension=2, tiled=True)
    query = opening_probe.reshape(seqs, heads, HEAD)
    query = lax.dynamic_slice_in_dim(query, first_row, rows, 2).astype(F32)
    read = lax.psum(jnp.einsum("shk,shkv->shv", query, final, precision=finest), "sp")
    read = read * lax.rsqrt(jnp.mean(read * read, axis=-1, keepdims=True) + 1e-06)
    return final.astype(BF16), read.reshape(seqs, heads * HEAD).astype(BF16)


def solution(mesh):
    in_specs = (
        P("grp", "sp", None),
        P(None, "tp"),
        P(None, "tp"),
        P(),
        P(),
        P("tp"),
        P("grp", "sp", "tp"),
        P("grp", "tp"),
    )
    out_specs = (P("grp", "tp", "sp", None), P("grp", "tp"))
    return jax.shard_map(body, mesh=mesh, in_specs=in_specs, out_specs=out_specs, check_vma=False)
```

```python
import functools
import math

import jax
import jax.numpy as jnp
from jax import lax
from jax.experimental import pallas as pl
from jax.experimental.pallas import tpu as pltpu
from jax.sharding import PartitionSpec as P

HEAD = 64
F32 = jnp.float32
BF16 = jnp.bfloat16

finest = lax.Precision.HIGHEST


def mm(left, right):
    return jnp.dot(left, right, preferred_element_type=F32)


def iota(shape, dim):
    return lax.broadcasted_iota(jnp.int32, shape, dim)


def onehot(flag):
    return jnp.where(flag, 1.0, 0.0).astype(BF16)


def lane_masks(pack, width):
    tile = min(128, width)
    lane_head = iota((1, tile), 1) // HEAD
    return [onehot(lane_head == h) for h in range(tile // HEAD)]


def blockdiag(member, masks):
    width = member.shape[1]
    tile = masks[0].shape[1]
    zeros = jnp.zeros((member.shape[0], tile), member.dtype)
    lines = []
    for head in range(width // HEAD):
        place = head * HEAD // tile
        pieces = [zeros] * (width // tile)
        pieces[place] = member[:, place * tile:(place + 1) * tile] * masks[head % len(masks)]
        lines.append(jnp.concatenate(pieces, axis=1))
    return jnp.concatenate(lines, axis=0)


def split(member):
    high = member.astype(BF16)
    return high, (member - high.astype(F32)).astype(BF16)


def thirds(member):
    high = member.astype(BF16)
    return (high,) + split(member - high.astype(F32))


def finish(masks, pack, sp, units, per, q_ref, ctx_ref, read_ref, maps, arrived, leaving,
           landed, reads, send_sem, recv_sem, send_out, recv_out):
    me = lax.axis_index("sp")
    rows = HEAD // sp
    width = pack * HEAD
    lines = width // 128
    eye = jnp.where(iota((HEAD, width), 0) == iota((HEAD, width), 1) % HEAD, 1.0, 0.0)
    quads = reads.shape[1] // width
    probe = q_ref[...].astype(F32)
    head_row = iota((8, width), 0)
    head_lane = iota((8, width), 1) // HEAD
    for i in range(per):
        for d in range(1, sp):
            peer_copy(maps.at[0], arrived.at[lax.rem(me + sp - d, sp), i], send_sem.at[0],
                      recv_sem.at[i, d], me).wait_recv()
        final = arrived[0, i, :HEAD, :]
        for j in range(1, sp):
            high, low = split(final)
            t_high, t_low = split(arrived[j, i, HEAD:, :])
            t_high = blockdiag(t_high, masks)
            final = (mm(high, t_high) + mm(low, t_high) + mm(high, blockdiag(t_low, masks))
                     + arrived[j, i, :HEAD, :])
        query = jnp.zeros((1, width), F32)
        for u in range(i, units, per):
            mine = jnp.where(u == me * per + i, 1.0, 0.0)
            at = (u % quads) * width
            query = query + mine * probe[u // quads:u // quads + 1, at:at + width]
        query = jnp.where(head_row == head_lane, query, 0.0)
        read = lax.dot_general(query, final, (((1,), (1,)), ((), ())), precision=finest,
                               preferred_element_type=F32)
        read = read * lax.rsqrt(jnp.mean(read * read, axis=1, keepdims=True) + 1e-06)
        read = jnp.dot(read, eye, precision=finest, preferred_element_type=F32)
        read = jnp.sum(jnp.where(head_row == head_lane, read, 0.0), axis=0, keepdims=True)
        turned = final.T
        for j in range(sp):
            for h in range(pack):
                leaving[i, j, h * rows:(h + 1) * rows, :HEAD] = (
                    turned[h * HEAD + j * rows:h * HEAD + (j + 1) * rows, :])
            for line in range(lines):
                leaving[i, j, pack * rows + line:pack * rows + line + 1, :] = (
                    read[:, line * 128:(line + 1) * 128])
        for d in range(1, sp):
            peer = lax.rem(me + d, sp)
            peer_copy(leaving.at[i, peer], landed.at[me * per + i], send_out.at[i, d],
                      recv_out.at[i, d], peer).start()
        landed[me * per + i] = leaving[i, me]
    for i in range(per):
        for d in range(1, sp):
            peer = lax.rem(me + sp - d, sp)
            peer_copy(leaving.at[i, 0], landed.at[peer * per + i], send_out.at[i, d],
                      recv_out.at[i, d], peer).wait_recv()
    for u in range(units):
        ctx_ref[u] = landed[u, :pack * rows, :HEAD].astype(BF16)
        for line in range(lines):
            at = (u % quads) * width + line * 128
            reads[u // quads:u // quads + 1, at:at + 128] = (
                landed[u, pack * rows + line:pack * rows + line + 1, :])
    read_ref[...] = reads[...].astype(BF16)
    for i in range(per):
        for d in range(1, sp):
            peer = lax.rem(me + d, sp)
            peer_copy(leaving.at[i, peer], landed.at[me * per + i], send_out.at[i, d],
                      recv_out.at[i, d], peer).wait_send()
    for u in range(units):
        @pl.when(u // per != me)
        def _():
            peer_copy(maps.at[u], arrived.at[me, u % per], send_sem.at[u],
                      recv_sem.at[u % per, 0], u // per).wait_send()


def peer_copy(source, target, send_sem, recv_sem, peer):
    return pltpu.make_async_remote_copy(
        src_ref=source, dst_ref=target, send_sem=send_sem, recv_sem=recv_sem,
        device_id={"sp": peer}, device_id_type=pl.DeviceIdType.MESH)


def local_stage(step, steps_per_seq, pack, x_ref, wk_ref, wv_ref, wb_ref, wf_ref, speed_ref,
                extra_ref, gate_weight, state):
    rows = x_ref.shape[0]
    columns = wk_ref.shape[1]
    heads = columns // HEAD
    width = pack * HEAD
    quads = columns // width
    chunks = rows // HEAD
    all_heads = wb_ref.shape[0]
    first_head = lax.axis_index("tp") * heads
    masks = lane_masks(pack, width)

    row_c = iota((HEAD, width), 0)
    lane_c = iota((HEAD, width), 1) % HEAD
    below = row_c > lane_c
    diagonal = row_c == lane_c
    apart = row_c ^ lane_c

    @pl.when(step == 0)
    def _():
        source = iota((128, all_heads), 1)
        lane = iota((128, all_heads), 0)
        to_beta = onehot((source == first_head + lane) & (lane < heads))
        to_decay = onehot((source == first_head + lane - heads) & (lane >= heads) & (lane < 2 * heads))
        gate_weight[...] = (mm(to_beta, wb_ref[...]) + mm(to_decay, wf_ref[...])).astype(BF16)

    @pl.when(lax.rem(step, steps_per_seq) == 0)
    def _():
        eye = jnp.where(diagonal, 1.0, 0.0)
        for quad in range(quads):
            state[quad, :HEAD, :] = jnp.zeros((HEAD, width), F32)
            state[quad, HEAD:, :] = eye

    x = x_ref[...]
    gates = lax.dot_general(x, gate_weight[...], (((1,), (1,)), ((), ())),
                            preferred_element_type=F32).astype(BF16)
    key_proj = mm(x, wk_ref[...]).astype(BF16).astype(F32)
    value_proj = mm(x, wv_ref[...]).astype(BF16).astype(F32)

    spread = iota((128, columns), 0)
    target = iota((128, columns), 1) // HEAD
    to_beta = onehot(spread == target)
    to_decay = onehot(spread == target + heads)
    place = iota((heads, 128), 0) + heads == iota((heads, 128), 1)
    raw = gates.astype(F32)
    softplus = jnp.maximum(raw, 0.0) + jnp.log1p(jnp.exp(-jnp.abs(raw)))
    speed = jnp.dot(-jnp.exp(speed_ref[...]), jnp.where(place, 1.0, 0.0),
                    precision=finest, preferred_element_type=F32)
    extra = lax.dot_general(extra_ref[0], onehot(place), (((0,), (0,)), ((), ())),
                            preferred_element_type=F32)
    gamma = speed * softplus + extra
    r_idx = iota((rows, rows), 0)
    c_idx = iota((rows, rows), 1)
    running = onehot((r_idx >= c_idx) & (r_idx // HEAD == c_idx // HEAD))
    cumul = sum(mm(running, piece) for piece in thirds(gamma))
    cumul = sum(mm(piece, to_decay) for piece in thirds(cumul))
    beta = sum(mm(piece, to_beta) for piece in split(jax.nn.sigmoid(raw)))

    key = key_proj * jax.nn.sigmoid(key_proj)
    value = value_proj * jax.nn.sigmoid(value_proj)
    group = onehot(iota((width, width), 0) // HEAD == iota((width, width), 1) // HEAD)
    squares = (key * key).astype(BF16)
    total = jnp.concatenate(
        [mm(squares[:, q * width:(q + 1) * width], group) for q in range(quads)], axis=1)
    key = key * lax.rsqrt(total + 1e-06)

    units = []
    for chunk in range(chunks):
        for quad in range(quads):
            units.append((slice(chunk * HEAD, (chunk + 1) * HEAD), slice(quad * width, (quad + 1) * width)))

    grown = jnp.exp(cumul)
    key16 = key.astype(BF16)
    weighted_key = (beta * grown * key).astype(BF16)
    weighted_value = (beta * value).astype(BF16)
    tile = masks[0].shape[1]
    eye16 = onehot(diagonal)
    levels = [onehot((apart >= 1 << p) & (apart < 2 << p)) for p in range(HEAD.bit_length() - 1)]
    contract = (((0,), (0,)), ((), ()))

    grams = []
    for rs, cs in units:
        grams.append(lax.dot_general(key16[rs, cs], blockdiag(key16[rs, cs], masks),
                                     (((1,), (1,)), ((), ())), preferred_element_type=F32))
    lowers = []
    for (rs, cs), gram in zip(units, grams):
        cum = cumul[rs, cs]
        across = jnp.sum(jnp.where(diagonal, cum, 0.0), axis=0, keepdims=True)
        weights = jnp.exp(jnp.where(below, cum - across, -1e30))
        lowers.append((beta[rs, cs] * gram * weights).astype(BF16))

    inverses = [eye16 - lower * levels[0] for lower in lowers]
    for level in levels[1:]:
        parts = [mm(inverse, blockdiag(lower * level, masks)).astype(BF16)
                 for lower, inverse in zip(lowers, inverses)]
        inverses = [inverse - mm(part, blockdiag(inverse, masks)).astype(BF16)
                    for inverse, part in zip(inverses, parts)]

    updates = [mm(inverse, blockdiag(weighted_value[rs, cs], masks)).astype(BF16)
               for (rs, cs), inverse in zip(units, inverses)]
    mixings = [mm(inverse, blockdiag(weighted_key[rs, cs], masks)).astype(BF16)
               for (rs, cs), inverse in zip(units, inverses)]
    closings, erases, offsets = [], [], []
    upper_lanes = iota((HEAD, tile), 1) >= HEAD
    for (rs, cs), update, mixing in zip(units, updates, mixings):
        last = cumul[rs, cs][HEAD - 1:HEAD, :]
        carried = (key[rs, cs] * jnp.exp(last - cumul[rs, cs])).astype(BF16)
        closings.append(jnp.exp(last))
        offset_tiles, erase_lines = [], []
        zeros = jnp.zeros((tile, tile), BF16)
        for place in range(width // tile):
            ts = slice(place * tile, (place + 1) * tile)
            offset = lax.dot_general(update[:, ts], carried[:, ts], contract, preferred_element_type=F32)
            erase = lax.dot_general(mixing[:, ts], carried[:, ts], contract, preferred_element_type=F32)
            if tile > HEAD:
                offset = jnp.where(upper_lanes, offset[HEAD:], offset[:HEAD])
            offset_tiles.append(offset)
            erase = erase.astype(BF16)
            erase = jnp.concatenate(
                [erase[h * HEAD:(h + 1) * HEAD] * masks[h] for h in range(tile // HEAD)], axis=0)
            line = [zeros] * (width // tile)
            line[place] = erase
            erase_lines.append(jnp.concatenate(line, axis=1))
        offsets.append(jnp.concatenate(offset_tiles, axis=1))
        erases.append(jnp.concatenate(erase_lines, axis=0))

    held = [(state[quad, :HEAD, :], state[quad, HEAD:, :]) for quad in range(quads)]
    for chunk in range(chunks):
        for quad in range(quads):
            u = chunk * quads + quad
            above, under = held[quad]
            erased = mm(jnp.concatenate([above, under], axis=0).astype(BF16), erases[u])
            held[quad] = (closings[u] * above - erased[:HEAD] + offsets[u],
                          closings[u] * under - erased[HEAD:])
    for quad in range(quads):
        state[quad, :HEAD, :], state[quad, HEAD:, :] = held[quad]


def local_kernel(steps_per_seq, pack, x_ref, wk_ref, wv_ref, wb_ref, wf_ref, speed_ref, extra_ref,
                 out_ref, gate_weight, state):
    step = pl.program_id(0)
    local_stage(step, steps_per_seq, pack, x_ref, wk_ref, wv_ref, wb_ref, wf_ref, speed_ref, extra_ref,
                gate_weight, state)

    @pl.when(lax.rem(step, steps_per_seq) == steps_per_seq - 1)
    def _():
        out_ref[0] = state[...]


def kernel(steps_per_seq, pack, sp, x_ref, wk_ref, wv_ref, wb_ref, wf_ref, speed_ref, extra_ref,
           q_ref, ctx_ref, read_ref, gate_weight, state, maps, arrived, leaving, landed, reads,
           send_sem, recv_sem, send_out, recv_out):
    step = pl.program_id(0)
    steps = pl.num_programs(0)
    me = lax.axis_index("sp")
    width = pack * HEAD
    quads = state.shape[0]
    masks = lane_masks(pack, width)

    @pl.when(step == 0)
    def _():
        barrier = pltpu.get_barrier_semaphore()
        for d in range(1, sp):
            pl.semaphore_signal(barrier, inc=1, device_id={"sp": lax.rem(me + d, sp)},
                                device_id_type=pl.DeviceIdType.MESH)

    local_stage(step, steps_per_seq, pack, x_ref, wk_ref, wv_ref, wb_ref, wf_ref, speed_ref, extra_ref,
                gate_weight, state)
    units_all = maps.shape[0]
    per = units_all // sp

    @pl.when(step == steps_per_seq - 1)
    def _():
        pl.semaphore_wait(pltpu.get_barrier_semaphore(), sp - 1)

    @pl.when(lax.rem(step, steps_per_seq) == steps_per_seq - 1)
    def _():
        seqs = units_all // quads
        seq = lax.rem(step // steps_per_seq + me * per // quads + 1, seqs)
        for quad in range(quads):
            unit = seq * quads + quad
            owner = unit // per
            slot = lax.rem(unit, per)

            @pl.when(owner != me)
            def _():
                maps[unit] = state[quad]
                away = lax.rem(owner - me + sp, sp)
                peer_copy(maps.at[unit], arrived.at[me, slot], send_sem.at[unit],
                          recv_sem.at[slot, away], owner).start()

            @pl.when(owner == me)
            def _():
                arrived[me, slot] = state[quad]

    @pl.when(step == steps - 1)
    def _():
        finish(masks, pack, sp, units_all, per, q_ref, ctx_ref, read_ref, maps, arrived,
               leaving, landed, reads, send_sem, recv_sem, send_out, recv_out)


def fused(layer_feed, address_mapping, content_mapping, beta_mapping_matrix, forgetting_mapping,
          logged_fading_speed, extra_forgetting, opening_probe):
    seqs, length, depth = layer_feed.shape
    columns = address_mapping.shape[1]
    heads = columns // HEAD
    pack = math.gcd(heads, 4)
    width = pack * HEAD
    quads = heads // pack
    units = seqs * quads
    sp = lax.axis_size("sp")
    per = units // sp
    rows = math.gcd(length, 4 * HEAD)
    per_seq = length // rows
    steps = seqs * per_seq
    all_heads = beta_mapping_matrix.shape[1]
    own_rows = HEAD // sp
    tall = -(-(pack * own_rows + width // 128) // 8) * 8
    whole = lambda shape: pl.BlockSpec(shape, lambda i: (0,) * len(shape), pipeline_mode=pl.Buffered(1))

    def turn(i):
        own = lax.axis_index("sp") * per // quads
        return (lax.rem(i + (own + 1) * per_seq, steps), 0)

    def turn_extra(i):
        block = turn(i)[0]
        return (block // per_seq, 0, lax.rem(block, per_seq))

    context, read = pl.pallas_call(
        functools.partial(kernel, per_seq, pack, sp),
        grid=(steps,),
        out_shape=(jax.ShapeDtypeStruct((units, pack * own_rows, HEAD), BF16),
                   jax.ShapeDtypeStruct((seqs, columns), BF16)),
        in_specs=[
            pl.BlockSpec((rows, depth), turn),
            whole((depth, columns)),
            whole((depth, columns)),
            whole((all_heads, depth)),
            whole((all_heads, depth)),
            whole((1, heads)),
            pl.BlockSpec((1, heads, rows), turn_extra),
            whole((seqs, columns)),
        ],
        out_specs=(pl.BlockSpec((units, pack * own_rows, HEAD), lambda i: (0, 0, 0)),
                   pl.BlockSpec((seqs, columns), lambda i: (0, 0))),
        scratch_shapes=[
            pltpu.VMEM((128, depth), BF16),
            pltpu.VMEM((quads, 2 * HEAD, width), F32),
            pltpu.VMEM((units, 2 * HEAD, width), F32),
            pltpu.VMEM((sp, per, 2 * HEAD, width), F32),
            pltpu.VMEM((per, sp, tall, 128), F32),
            pltpu.VMEM((units, tall, 128), F32),
            pltpu.VMEM((seqs, columns), F32),
            pltpu.SemaphoreType.DMA((units,)),
            pltpu.SemaphoreType.DMA((per, sp)),
            pltpu.SemaphoreType.DMA((per, sp)),
            pltpu.SemaphoreType.DMA((per, sp)),
        ],
        compiler_params=pltpu.CompilerParams(
            dimension_semantics=("arbitrary",), vmem_limit_bytes=56 * 2**20,
            collective_id=0, has_side_effects=True),
    )(layer_feed.reshape(seqs * length, depth), address_mapping, content_mapping,
      beta_mapping_matrix.T, forgetting_mapping.T, logged_fading_speed[None, :],
      extra_forgetting.transpose(0, 2, 1),
      opening_probe)
    return context.reshape(seqs, heads, own_rows, HEAD), read


def device_maps(layer_feed, address_mapping, content_mapping, beta_mapping_matrix,
                forgetting_mapping, logged_fading_speed, extra_forgetting):
    seqs, length, depth = layer_feed.shape
    columns = address_mapping.shape[1]
    heads = columns // HEAD
    pack = math.gcd(heads, 4)
    width = pack * HEAD
    quads = heads // pack
    rows = math.gcd(length, 4 * HEAD)
    per_seq = length // rows
    all_heads = beta_mapping_matrix.shape[1]
    whole = lambda shape: pl.BlockSpec(shape, lambda i: (0, 0), pipeline_mode=pl.Buffered(1))
    return pl.pallas_call(
        functools.partial(local_kernel, per_seq, pack),
        grid=(seqs * per_seq,),
        out_shape=jax.ShapeDtypeStruct((seqs, quads, 2 * HEAD, width), F32),
        in_specs=[
            pl.BlockSpec((rows, depth), lambda i: (i, 0)),
            whole((depth, columns)),
            whole((depth, columns)),
            whole((all_heads, depth)),
            whole((all_heads, depth)),
            whole((1, heads)),
            pl.BlockSpec((1, heads, rows), lambda i: (i // per_seq, 0, i % per_seq)),
        ],
        out_specs=pl.BlockSpec((1, quads, 2 * HEAD, width), lambda i: (i // per_seq, 0, 0, 0)),
        scratch_shapes=[
            pltpu.VMEM((128, depth), BF16),
            pltpu.VMEM((quads, 2 * HEAD, width), F32),
        ],
        compiler_params=pltpu.CompilerParams(
            dimension_semantics=("arbitrary",), vmem_limit_bytes=56 * 2**20),
    )(layer_feed.reshape(seqs * length, depth), address_mapping, content_mapping,
      beta_mapping_matrix.T, forgetting_mapping.T, logged_fading_speed[None, :], extra_forgetting.transpose(0, 2, 1))


def matmul(left, right):
    return jnp.einsum("shij,shjk->shik", left, right, precision=finest)


def suffix_product(part, axis):
    count = lax.axis_size(axis)
    ahead = count - 1 - lax.axis_index(axis)
    gathered = lax.all_gather(part, axis)
    start = jnp.broadcast_to(jnp.eye(HEAD, dtype=F32), part.shape)

    def one(hop, carry):
        return matmul(carry, lax.dynamic_index_in_dim(gathered, count - 1 - hop, 0, False))

    return lax.fori_loop(0, ahead, one, start)


def body(layer_feed, address_mapping, content_mapping, beta_mapping_matrix, forgetting_mapping,
         logged_fading_speed, extra_forgetting, opening_probe):
    seqs = layer_feed.shape[0]
    heads = address_mapping.shape[1] // HEAD
    sp = lax.axis_size("sp")
    pack = math.gcd(heads, 4)
    if pack > 1 and (seqs * heads // pack) % sp == 0 and HEAD % (8 * sp) == 0:
        return fused(layer_feed, address_mapping, content_mapping, beta_mapping_matrix,
                     forgetting_mapping, logged_fading_speed, extra_forgetting, opening_probe)
    maps = device_maps(layer_feed, address_mapping, content_mapping, beta_mapping_matrix,
                       forgetting_mapping, logged_fading_speed, extra_forgetting)
    quads, width = maps.shape[1], maps.shape[3]
    maps = maps.reshape(seqs, quads, 2, HEAD, width // HEAD, HEAD)
    maps = maps.transpose(2, 0, 1, 4, 5, 3).reshape(2, seqs, heads, HEAD, HEAD)
    offset, transfer = maps[0], maps[1]
    rows = HEAD // lax.axis_size("sp")
    first_row = lax.axis_index("sp") * rows
    terms = matmul(suffix_product(transfer, "sp"), offset)
    final = lax.psum_scatter(terms, "sp", scatter_dimension=2, tiled=True)
    query = opening_probe.reshape(seqs, heads, HEAD)
    query = lax.dynamic_slice_in_dim(query, first_row, rows, 2).astype(F32)
    read = lax.psum(jnp.einsum("shk,shkv->shv", query, final, precision=finest), "sp")
    read = read * lax.rsqrt(jnp.mean(read * read, axis=-1, keepdims=True) + 1e-06)
    return final.astype(BF16), read.reshape(seqs, heads * HEAD).astype(BF16)


def solution(mesh):
    in_specs = (
        P("grp", "sp", None),
        P(None, "tp"),
        P(None, "tp"),
        P(),
        P(),
        P("tp"),
        P("grp", "sp", "tp"),
        P("grp", "tp"),
    )
    out_specs = (P("grp", "tp", "sp", None), P("grp", "tp"))
    return jax.shard_map(body, mesh=mesh, in_specs=in_specs, out_specs=out_specs, check_vma=False)
```
